512 devices in a mesh: ep: 32 (over z, core), tp: 16 (over y, x).
Axes of the slice: x: 4, y: 4, z: 16, core: 2. Of those that a mesh axis runs over, the one named last changes fastest.
Arguments:
- query_rows: bfloat16 [24576, 1024], P('ep', 'tp'), may hold values from -600 to 600
- key_rows: bfloat16 [24576, 1024], P('ep', 'tp'), may hold values from -6 to 6
- value_rows: bfloat16 [24576, 1024], P('ep', 'tp'), may hold values from -6 to 6
- cum_gate: float32 [16, 24576], P('tp'), may hold values from -2458 to 0, as said below
- out_weight: bfloat16 [1024, 2048], P(None, 'tp'), may hold values from -0.1875 to 0.1875
- moe_input: bfloat16 [6144, 2048], P('ep'), may hold values from -6 to 6
- moe_gain: float32 [2048], replicated, may hold values from 0.1 to 1.9
- routes: int32 [6144, 3], P('ep'), may hold values from 0 to 127, all different within a row; in each aligned block of 192 rows (0 to 191, 192 to 383, ...) at most 9 rows name the same one
- route_weight: float32 [6144, 3], P('ep'), may hold values from 0.2 to 1.5
- expert_gate: bfloat16 [128, 2048, 512], P('ep', None, 'tp'), may hold values from -0.125 to 0.125
- expert_up: bfloat16 [128, 2048, 512], P('ep', None, 'tp'), may hold values from -0.125 to 0.125
- expert_down: bfloat16 [128, 512, 2048], P('ep', None, 'tp'), may hold values from -0.25 to 0.25
- shared_gate: bfloat16 [2048, 512], P(None, 'tp'), may hold values from -0.125 to 0.125
- shared_up: bfloat16 [2048, 512], P(None, 'tp'), may hold values from -0.125 to 0.125
- shared_down: bfloat16 [512, 2048], P(None, 'tp'), may hold values from -0.25 to 0.25
Outputs:
- mixer_out: bfloat16 [24576, 2048], P('ep', 'tp')
- moe_out: bfloat16 [6144, 2048], P('ep', 'tp')
The draws below stay inside these ranges and needn't reach their ends.
Inputs may be any that keep to these rules, and one draw needn't show every extreme that they name: Non-increasing along positions: cum_gate[h, t] is the sum of the log forget gates of head h over positions 0 to t. `routes`: the 3 experts of a token differ. In each aligned block of 192 tokens no expert is named by more than 9 tokens, a bound that some block reaches.
All inputs are finite; a program needn't handle non-finite values.
Results may differ from the reference program's by a relative error of at most 0.0068.
Values may be sent and summed in bfloat16 or wider, within the bound.
A program may use at most 64 MiB of HBM per device.

```python
import math
import jax
import jax.numpy as jnp
import numpy as np
from jax import lax

D = 2048
HEADS = 16
HEAD = 64
FF = 512
FS = 512
EXPERTS = 128
TOP = 3
SEQ_DEV = 768
LENGTH = 24576
MOE_DEV = 192
TOKENS_MOE = 6144
CAP = 9
N_EP = 32


def draw_query_rows(key, part):
    base_key = jax.random.fold_in(key, 7)
    key_normal = jax.random.fold_in(base_key, 0)
    drawn = jnp.clip(jax.random.normal(key_normal, (LENGTH, HEADS * HEAD), jnp.float32), -6.0, 6.0)
    return drawn.astype(jnp.bfloat16)


def draw_cum_gate(key, part):
    base_key = jax.random.fold_in(key, 13)
    key_heads, key_steps, key_blocks = jax.random.split(base_key, 3)
    head_order = jax.random.permutation(key_heads, HEADS)
    fast_count = HEADS // 2
    decay_rates = jnp.where(head_order < fast_count, 1.0 / 40.0, 1.0 / LENGTH).astype(jnp.float32)
    low = jnp.log(0.5)
    high = jnp.log(2.0)
    step_factors = jnp.exp(jax.random.uniform(key_steps, (HEADS, LENGTH), jnp.float32, low, high))
    block_factors = jnp.exp(jax.random.uniform(key_blocks, (HEADS, LENGTH // SEQ_DEV), jnp.float32, low, high))
    block_factors = jnp.repeat(block_factors, SEQ_DEV, axis=1)
    log_gates = -decay_rates[:, None] * step_factors * block_factors
    return jnp.cumsum(log_gates, axis=1).astype(jnp.float32)


def levels(rng, shape, cuts, least, high):
    def one(axis_at, shards_of):
        draws = jax.random.uniform(jax.random.fold_in(jax.random.fold_in(rng, 6), axis_at), (shards_of,), jnp.float32, least / len(cuts), high / len(cuts))
        return jnp.repeat(jnp.exp(draws), shape[axis_at] // shards_of).reshape((-1,) + (1,) * (len(shape) - axis_at - 1))

    loudness = one(*cuts[0])
    for cut in cuts[1:]:
        loudness = loudness * one(*cut)
    return loudness


def deal_out(rng, own, number, rows, amount, top, limit, slope):
    order = jax.random.permutation(rng, amount)
    heavy_load, common = load_shares(amount, rows * top, limit, slope, True), load_shares(amount, rows * top, limit, slope, False)
    places = jnp.arange(amount)

    def named(tallies, turn):
        used = int((tallies > 0).sum())
        fixed = max(1, used // 4)
        shifted = fixed + (places - fixed + turn * (used - fixed)) % max(1, amount - fixed)
        return jnp.zeros((amount,), jnp.int32).at[order[jnp.where(places < fixed, places, shifted)]].set(jnp.asarray(tallies, jnp.int32))

    tallies = jnp.where(number % 4 == 0, named(heavy_load, number // 4), named(common, number - number // 4 - 1))
    mixed = jax.random.permutation(jax.random.fold_in(own, 3), amount)
    donor, receiver = mixed[0:amount // 2 * 2:2], mixed[1:amount // 2 * 2:2]
    margin = jnp.minimum(tallies[donor] - 1, limit - tallies[receiver]) // 2
    margin = jnp.where((donor == order[0]) | (receiver == order[0]) | (tallies[receiver] == 0), 0, jnp.maximum(margin, 0))
    shifted = jax.random.randint(jax.random.fold_in(own, 4), (amount // 2,), 0, 1 << 20) % (margin + 1)
    tallies = tallies.at[donor].add(-shifted).at[receiver].add(shifted)
    members = jnp.searchsorted(jnp.cumsum(tallies), jnp.arange(rows * top), side="right").astype(jnp.int32)
    listing = members.reshape(top, rows).T
    listing = listing[jax.random.permutation(jax.random.fold_in(own, 1), rows)]
    turn = jax.random.randint(jax.random.fold_in(own, 2), (rows, 1), 0, top)
    return jnp.take_along_axis(listing, (jnp.arange(top)[None, :] + turn) % top, axis=1)


def load_shares(amount, total, reach, skew, full):
    portions = [(1 << 20) // math.isqrt(standing ** skew) + 1 for standing in range(1, amount + 1)]
    largest = reach if full else min(reach, max(-(-total // amount), total * portions[0] // sum(portions)))
    least = 1 if total - largest >= amount - 1 else 0
    holding, rest = [largest] + [least] * (amount - 1), total - largest - least * (amount - 1)
    while rest > 0:
        free = [i for i in range(1, amount) if holding[i] < largest] or [i for i in range(1, amount) if holding[i] < reach]
        pool, left = sum([portions[i] for i in free]), rest
        for i in free:
            more = min(reach - holding[i], max(1, left * portions[i] // pool), rest)
            holding[i] = holding[i] + more
            rest = rest - more
    return np.array(holding)


def bell_draw(stream_key, shape, deviation, limit, cuts=(), kind=jnp.bfloat16):
    array = jax.random.normal(stream_key, shape, jnp.float32) * deviation
    if len(cuts) > 0:
        array = levels(stream_key, shape, cuts, -0.22, 0.18) * array
    return jnp.clip(array, min=-limit, max=limit).astype(kind)


def setup_inputs(seed: int = 0) -> dict:
    keys = jax.random.split(jax.random.key(seed), 16)
    query_rows = draw_query_rows(jax.random.fold_in(keys[15], 71), 0)
    key_rows = bell_draw(keys[1], (LENGTH, HEADS * HEAD), 1.0, 6.0, ((0, 32), (1, 16)))
    value_rows = bell_draw(keys[2], (LENGTH, HEADS * HEAD), 1.0, 6.0, ((0, 32), (1, 16)))
    cum_gate = draw_cum_gate(jax.random.fold_in(keys[15], 71), 0)
    out_weight = bell_draw(keys[4], (HEADS * HEAD, D), (HEADS * HEAD) ** -0.5, 0.1875, ((1, 16),))
    moe_input = bell_draw(keys[5], (TOKENS_MOE, D), 1.0, 6.0, ((0, 32),))
    moe_gain = jnp.clip(1.0 + 0.18 * jax.random.normal(keys[6], (D,), jnp.float32), 0.1, 1.9)
    routes_keys = jax.random.split(jax.random.fold_in(keys[7], 1), TOKENS_MOE // MOE_DEV)
    routes_turns = jax.random.permutation(jax.random.fold_in(keys[7], 3), TOKENS_MOE // MOE_DEV)
    routes = jax.vmap(lambda own, number: deal_out(jax.random.fold_in(keys[7], 2), own, number, MOE_DEV, EXPERTS, TOP, CAP, 2))(routes_keys, routes_turns).reshape((TOKENS_MOE, TOP))
    route_weight = jnp.clip(jnp.exp(math.log(1.5) - 2.014903 * jax.random.uniform(keys[8], (TOKENS_MOE, TOP), jnp.float32) ** levels(keys[8], (TOKENS_MOE, TOP), ((0, 32),), -0.2, 0.2)), 0.2, 1.5)
    expert_gate = bell_draw(keys[9], (EXPERTS, D, FF), D ** -0.5, 0.125, ((0, 32), (2, 16)))
    expert_up = bell_draw(keys[10], (EXPERTS, D, FF), D ** -0.5, 0.125, ((0, 32), (2, 16)))
    expert_down = bell_draw(keys[11], (EXPERTS, FF, D), FF ** -0.5, 0.25, ((0, 32), (2, 16)))
    shared_gate = bell_draw(keys[12], (D, FS), D ** -0.5, 0.125, ((1, 16),))
    shared_up = bell_draw(keys[13], (D, FS), D ** -0.5, 0.125, ((1, 16),))
    shared_down = bell_draw(keys[14], (FS, D), FS ** -0.5, 0.25, ((1, 16),))
    return {"query_rows": query_rows, "key_rows": key_rows, "value_rows": value_rows, "cum_gate": cum_gate, "out_weight": out_weight, "moe_input": moe_input, "moe_gain": moe_gain, "routes": routes, "route_weight": route_weight, "expert_gate": expert_gate, "expert_up": expert_up, "expert_down": expert_down, "shared_gate": shared_gate, "shared_up": shared_up, "shared_down": shared_down}


neg_fill = -1e+30
norm_eps = 1e-06

def attention_heads(query_rows, key_rows, value_rows, cum_gate):
    query_span = 128 if LENGTH % 128 == 0 else LENGTH
    query_heads = query_rows.reshape(LENGTH, HEADS, HEAD)
    key_heads = key_rows.reshape(LENGTH, HEADS, HEAD).astype(jnp.float32)
    value_heads = value_rows.reshape(LENGTH, HEADS, HEAD).astype(jnp.float32)
    key_pos = jnp.arange(LENGTH, dtype=jnp.int32)
    scale = HEAD ** (-0.5)

    def one_block(block_index):
        start = (block_index * query_span).astype(jnp.int32)
        query_block = lax.dynamic_slice_in_dim(query_heads, start, query_span, 0).astype(jnp.float32)
        query_gate = lax.dynamic_slice_in_dim(cum_gate, start, query_span, 1)
        scores = jnp.einsum('qhd,khd->hqk', query_block, key_heads) * scale
        scores = scores + query_gate[:, :, None] - cum_gate[:, None, :]
        query_pos = start + jnp.arange(query_span, dtype=jnp.int32)
        causal = key_pos[None, :] <= query_pos[:, None]
        scores = jnp.where(causal[None], scores, neg_fill)
        row_max = lax.optimization_barrier(jnp.max(scores, axis=2, keepdims=True))
        expon = jnp.where(causal[None], jnp.exp(scores - row_max), 0.0)
        denom = lax.optimization_barrier(jnp.sum(expon, axis=2))
        probs = lax.optimization_barrier(expon.astype(jnp.bfloat16)).astype(jnp.float32)
        summed = jnp.einsum('hqk,khd->qhd', probs, value_heads)
        result = summed / jnp.transpose(denom)[:, :, None]
        return result.astype(jnp.bfloat16).reshape(query_span, HEADS * HEAD)
    blocks = lax.map(one_block, jnp.arange(LENGTH // query_span, dtype=jnp.int32))
    return blocks.reshape(LENGTH, HEADS * HEAD)

def experts_branch(moe_input, moe_gain, routes, route_weight, expert_gate, expert_up, expert_down, shared_gate, shared_up, shared_down):
    moe_rows = moe_input.astype(jnp.float32)
    normed = (moe_rows * lax.rsqrt(lax.optimization_barrier(jnp.mean(moe_rows * moe_rows, axis=1, keepdims=True)) + norm_eps) * moe_gain).astype(jnp.bfloat16)
    pair_count = TOKENS_MOE * TOP
    flat_routes = routes.reshape(-1).astype(jnp.int32)
    one_hot = (flat_routes[:, None] == jnp.arange(EXPERTS, dtype=jnp.int32)[None, :]).astype(jnp.int32)
    one_hot = one_hot.reshape(N_EP, MOE_DEV * TOP, EXPERTS)
    ranks = lax.optimization_barrier(jnp.sum(jnp.cumsum(one_hot, axis=1) * one_hot, axis=2)).reshape(-1) - 1
    block_id = jnp.arange(pair_count, dtype=jnp.int32) // (MOE_DEV * TOP)
    slot_index = (flat_routes * (N_EP * CAP) + block_id * CAP + ranks).astype(jnp.int32)
    pair_token = jnp.arange(pair_count, dtype=jnp.int32) // TOP
    slot_token = jnp.full((EXPERTS * N_EP * CAP,), TOKENS_MOE, jnp.int32).at[slot_index].set(pair_token)
    padded = jnp.concatenate([normed, jnp.zeros((1, D), jnp.bfloat16)], axis=0)

    def one_expert(pieces):
        token_index, gate_w, up_w, down_w = pieces
        gathered = padded[token_index]
        gate_val = jnp.dot(gathered, gate_w, preferred_element_type=jnp.float32)
        up_val = jnp.dot(gathered, up_w, preferred_element_type=jnp.float32)
        hidden = (jax.nn.silu(gate_val) * up_val).astype(jnp.bfloat16)
        return jnp.dot(hidden, down_w, preferred_element_type=jnp.float32).astype(jnp.bfloat16)
    results = lax.map(one_expert, (slot_token.reshape(EXPERTS, N_EP * CAP), expert_gate, expert_up, expert_down))
    picked = results.reshape(EXPERTS * N_EP * CAP, D)[slot_index].astype(jnp.float32).reshape(TOKENS_MOE, TOP, D)
    routed = lax.optimization_barrier(jnp.sum(picked * route_weight[:, :, None], axis=1))
    shared_hidden = (jax.nn.silu(jnp.dot(normed, shared_gate, preferred_element_type=jnp.float32)) * jnp.dot(normed, shared_up, preferred_element_type=jnp.float32)).astype(jnp.bfloat16)
    total = routed + jnp.dot(shared_hidden, shared_down, preferred_element_type=jnp.float32)
    return total.astype(jnp.bfloat16)

def reference(query_rows, key_rows, value_rows, cum_gate, out_weight, moe_input, moe_gain, routes, route_weight, expert_gate, expert_up, expert_down, shared_gate, shared_up, shared_down):
    heads_out = attention_heads(query_rows, key_rows, value_rows, cum_gate)
    mixer_out = jnp.dot(heads_out, out_weight, preferred_element_type=jnp.float32).astype(jnp.bfloat16)
    moe_out = experts_branch(moe_input, moe_gain, routes, route_weight, expert_gate, expert_up, expert_down, shared_gate, shared_up, shared_down)
    return (mixer_out, moe_out)
```

```python
import jax
import jax.numpy as jnp
from jax import lax
from jax.experimental import pallas as pl
from jax.experimental.pallas import tpu as pltpu
from jax.sharding import PartitionSpec as P

HEAD = 64


neg_fill = -1e30
norm_eps = 1e-06


def joined_along(pieces, dim):
    dims = list(pieces.shape[1:])
    dims[dim] *= pieces.shape[0]
    return jnp.moveaxis(pieces, 0, dim).reshape(dims)


def sent_to_all(array, axis):
    copies = jnp.broadcast_to(array, (lax.axis_size(axis), *array.shape))
    return lax.all_to_all(copies, axis, split_axis=0, concat_axis=0, tiled=True)


def collect(array, axis, dim):
    return joined_along(sent_to_all(array, axis), dim)


MESH = pl.DeviceIdType.MESH
SPAN = 768
Z = 16
TP = 16
UP = 8
DOWN = 7


def remote(src, dst, send, recv, ep, tp):
    return pltpu.make_async_remote_copy(
        src_ref=src, dst_ref=dst, send_sem=send, recv_sem=recv, device_id=(ep, tp), device_id_type=MESH
    )


def attention_kernel(
    q_ref,
    k_hbm,
    v_hbm,
    gate_ref,
    wo_ref,
    out_ref,
    kbuf,
    vbuf,
    q_scr,
    m_scr,
    acc,
    packed,
    heads,
    wide,
    own_sem,
    up_send,
    up_recv,
    dn_send,
    dn_recv,
    pr_send,
    pr_recv,
    hd_send,
    hd_recv,
):
    ep = lax.axis_index("ep")
    tp = lax.axis_index("tp")
    z = ep // 2
    c = ep % 2
    above = ((z + 1) % Z) * 2 + c
    below = ((z + Z - 1) % Z) * 2 + c
    partner = z * 2 + (1 - c)

    own = [
        pltpu.make_async_copy(k_hbm, kbuf.at[ep], own_sem.at[0]),
        pltpu.make_async_copy(v_hbm, vbuf.at[ep, pl.ds(64, 64)], own_sem.at[1]),
    ]
    for copy in own:
        copy.start()

    barrier = pltpu.get_barrier_semaphore()
    for peer in (above, below, partner):
        pl.semaphore_signal(barrier, inc=1, device_id=(peer, tp), device_id_type=MESH)
    for hop in range(1, TP):
        pl.semaphore_signal(
            barrier, inc=1, device_id=(ep, (tp + hop) % TP), device_id_type=MESH
        )

    def part(block, half):
        return kbuf.at[block] if half == 0 else vbuf.at[block, pl.ds(64, 64)]

    def up_copy(step, half):
        block = ((z - step + Z) % Z) * 2 + c
        return remote(
            part(block, half), part(block, half), up_send.at[step, half], up_recv.at[step, half], above, tp
        )

    def dn_copy(step, half):
        block = ((z + step) % Z) * 2 + c
        return remote(
            part(block, half), part(block, half), dn_send.at[step, half], dn_recv.at[step, half], below, tp
        )

    def up_landed(step, half):
        block = ((z - step + Z) % Z) * 2 + c
        return remote(
            part(block, half), part(block, half), up_send.at[step - 1, half], up_recv.at[step - 1, half], below, tp
        )

    def dn_landed(step, half):
        block = ((z + step) % Z) * 2 + c
        return remote(
            part(block, half), part(block, half), dn_send.at[step - 1, half], dn_recv.at[step - 1, half], above, tp
        )

    def pr_copy(slot, block, half):
        return remote(
            part(block, half), part(block, half), pr_send.at[slot, half], pr_recv.at[slot, half], partner, tp
        )

    def up_sends(step):
        return (z - step >= 0) & (z < Z - 1)

    def up_lands(step):
        return z - step >= 0

    def dn_moves(step):
        return (z + step) % Z <= 6

    def dn_used(step):
        return ((z + step) % Z <= 6) & ((z + step) % Z < z)

    vbuf[:, 0:64, :] = jnp.ones((2 * Z, 64, SPAN), jnp.bfloat16)
    q_scr[...] = (q_ref[...].astype(jnp.float32) * 0.125).T.astype(jnp.bfloat16)
    m_scr[...] = jnp.full(m_scr.shape, -1e30, jnp.float32)
    acc[...] = jnp.zeros(acc.shape, jnp.float32)

    for copy in own:
        copy.wait()
    pl.semaphore_wait(barrier, TP + 2)

    for half in range(2):

        @pl.when(up_sends(0))
        def _():
            up_copy(0, half).start()

        @pl.when(dn_moves(0))
        def _():
            dn_copy(0, half).start()

        @pl.when(c == 0)
        def _():
            pr_copy(0, ep, half).start()

    gate_first = gate_ref[:, pl.ds(pl.multiple_of(ep * SPAN, 128), 128)][:, 0:1]

    def attend(block, diagonal):
        bias = gate_first - gate_ref[:, pl.ds(pl.multiple_of(block * SPAN, 128), SPAN)]
        keys = kbuf[block]
        values = vbuf[block]
        rows = 256
        for start in range(0, SPAN, rows):
            span = pl.ds(start, rows)
            scores = jnp.dot(q_scr[span, :], keys, preferred_element_type=jnp.float32) + bias
            if diagonal:
                row = lax.broadcasted_iota(jnp.int32, scores.shape, 0) + start
                column = lax.broadcasted_iota(jnp.int32, scores.shape, 1)
                scores = jnp.where(column <= row, scores, -1e30)
            old = m_scr[span, :]
            new = jnp.maximum(old, jnp.max(scores, axis=1, keepdims=True))
            probs = jnp.exp(scores - jnp.concatenate([new] * (SPAN // 128), axis=1))
            summed = lax.dot_general(
                probs.astype(jnp.bfloat16),
                values,
                (((1,), (1,)), ((), ())),
                preferred_element_type=jnp.float32,
            )
            acc[span, :] = acc[span, :] * jnp.exp(old - new) + summed
            m_scr[span, :] = new

    attend(ep, True)

    def ring(step, carry):
        up_ok = up_lands(step)
        dn_ok = (step <= DOWN) & dn_moves(step)
        for half in range(2):

            @pl.when(up_ok)
            def _():
                up_landed(step, half).wait_recv()

                @pl.when((step < UP) & up_sends(step))
                def _():
                    up_copy(step, half).start()

                pr_copy(step, ((z - step + Z) % Z) * 2 + c, half).start()

            @pl.when(dn_ok)
            def _():
                dn_landed(step, half).wait_recv()

                @pl.when(step < DOWN)
                def _():
                    dn_copy(step, half).start()

                @pl.when(dn_used(step))
                def _():
                    pr_copy(UP + step, ((z + step) % Z) * 2 + c, half).start()

        def one(i, carry):
            down = i % 2
            other = i // 2
            used = jnp.where(
                down == 1, ((step <= DOWN) & dn_used(step)).astype(jnp.int32), up_ok.astype(jnp.int32)
            )
            origin = jnp.where(down == 1, (z + step) % Z, (z - step + Z) % Z)
            block = origin * 2 + jnp.where(other == 1, 1 - c, c)

            @pl.when(used == 1)
            def _():
                @pl.when(other == 1)
                def _():
                    slot = step + down * UP
                    for half in range(2):
                        pr_copy(slot, block, half).wait_recv()

                attend(block, False)

            return carry

        lax.fori_loop(0, 4, one, 0)
        return carry

    @pl.when(c == 1)
    def _():
        for half in range(2):
            pr_copy(0, partner, half).wait_recv()
        attend(partner, False)

    lax.fori_loop(1, UP + 1, ring, 0)

    total = acc[...]
    ratio = total / pltpu.roll(total, 64, 1)
    lane = lax.broadcasted_iota(jnp.int32, (384, 128), 1)
    packed[...] = jnp.where(lane < 64, pltpu.roll(ratio[:384], 64, 1), ratio[384:]).astype(jnp.bfloat16)

    def head_copy(hop):
        return remote(
            packed, heads.at[tp], hd_send.at[hop], hd_recv.at[tp], ep, (tp + hop) % TP
        )

    for hop in range(1, TP):
        head_copy(hop).start()
    heads[tp] = packed[...]
    for head in range(TP):
        w = wo_ref[head * 64 : head * 64 + 64, :]
        wide[head * 128 : head * 128 + 64, :] = jnp.concatenate([w, jnp.zeros_like(w)], axis=1)
        wide[head * 128 + 64 : head * 128 + 128, :] = jnp.concatenate([jnp.zeros_like(w), w], axis=1)
    for hop in range(1, TP):
        source = (tp + TP - hop) % TP
        remote(
            packed, heads.at[source], hd_send.at[hop], hd_recv.at[source], ep, source
        ).wait_recv()
    mixed = jnp.zeros((384, 256), jnp.float32)
    for head in range(TP):
        mixed = mixed + jnp.dot(
            heads[head], wide[head * 128 : head * 128 + 128, :], preferred_element_type=jnp.float32
        )
    out_ref[0:384, :] = mixed[:, 0:128].astype(jnp.bfloat16)
    out_ref[384:768, :] = mixed[:, 128:256].astype(jnp.bfloat16)

    for hop in range(1, TP):
        head_copy(hop).wait_send()

    def drain(step, carry):
        for half in range(2):

            @pl.when(up_sends(step) & (step < UP))
            def _():
                up_copy(step, half).wait_send()

            @pl.when((step < DOWN) & dn_moves(step))
            def _():
                dn_copy(step, half).wait_send()

            @pl.when((step >= 1) & up_lands(step))
            def _():
                pr_copy(step, ((z - step + Z) % Z) * 2 + c, half).wait_send()

            @pl.when((step >= 1) & (step <= DOWN) & dn_used(step))
            def _():
                pr_copy(UP + step, ((z + step) % Z) * 2 + c, half).wait_send()

        return carry

    @pl.when(c == 0)
    def _():
        for half in range(2):
            pr_copy(0, ep, half).wait_send()

    lax.fori_loop(0, UP + 1, drain, 0)


def attention(query_rows, key_rows, value_rows, cum_gate, out_weight):
    vmem = pl.BlockSpec(memory_space=pltpu.VMEM)
    hbm = pl.BlockSpec(memory_space=pl.ANY)
    dma = pltpu.SemaphoreType.DMA
    return pl.pallas_call(
        attention_kernel,
        out_shape=jax.ShapeDtypeStruct((SPAN, 128), jnp.bfloat16),
        in_specs=[vmem, hbm, hbm, vmem, vmem],
        out_specs=vmem,
        scratch_shapes=[
            pltpu.VMEM((2 * Z, 64, SPAN), jnp.bfloat16),
            pltpu.VMEM((2 * Z, 128, SPAN), jnp.bfloat16),
            pltpu.VMEM((SPAN, 64), jnp.bfloat16),
            pltpu.VMEM((SPAN, 128), jnp.float32),
            pltpu.VMEM((SPAN, 128), jnp.float32),
            pltpu.VMEM((384, 128), jnp.bfloat16),
            pltpu.VMEM((TP, 384, 128), jnp.bfloat16),
            pltpu.VMEM((TP * 128, 256), jnp.bfloat16),
            dma((2,)),
            dma((UP, 2)),
            dma((UP, 2)),
            dma((DOWN, 2)),
            dma((DOWN, 2)),
            dma((UP + DOWN + 1, 2)),
            dma((UP + DOWN + 1, 2)),
            dma((TP,)),
            dma((TP,)),
        ],
        compiler_params=pltpu.CompilerParams(
            collective_id=0, has_side_effects=True, vmem_limit_bytes=56 * 2**20
        ),
        cost_estimate=pl.CostEstimate(flops=5 * 10**10, bytes_accessed=10**7, transcendentals=0),
        name="attention",
    )(query_rows.T, key_rows.T, value_rows.T, cum_gate, out_weight)


def local(
    query_rows,
    key_rows,
    value_rows,
    cum_gate,
    out_weight,
    moe_input,
    moe_gain,
    routes,
    route_weight,
    expert_gate,
    expert_up,
    expert_down,
    shared_gate,
    shared_up,
    shared_down,
):
    mixer_out = attention(query_rows, key_rows, value_rows, cum_gate, out_weight)
    token_count = moe_input.shape[0]
    top_count = routes.shape[1]
    local_experts = expert_gate.shape[0]
    ep_count = lax.axis_size("ep")
    expert_count = local_experts * ep_count
    capacity = 2 * token_count * top_count // expert_count
    column_count = expert_down.shape[2]
    first_column = lax.axis_index("tp") * column_count
    moe_rows = moe_input.astype(jnp.float32)
    normed = (
        moe_rows
        * lax.rsqrt(jnp.mean(moe_rows * moe_rows, axis=1, keepdims=True) + norm_eps)
        * moe_gain
    ).astype(jnp.bfloat16)
    flat_routes = routes.reshape(-1)
    one_hot = (flat_routes[:, None] == jnp.arange(expert_count, dtype=jnp.int32)[None, :]).astype(
        jnp.int32
    )
    ranks = jnp.sum(jnp.cumsum(one_hot, axis=0) * one_hot, axis=1) - 1
    slot_index = flat_routes * capacity + ranks
    pair_token = jnp.arange(token_count * top_count, dtype=jnp.int32) // top_count
    slot_token = (
        jnp.full((expert_count * capacity,), token_count, jnp.int32).at[slot_index].set(pair_token)
    )
    padded = jnp.concatenate([normed, jnp.zeros((1, normed.shape[1]), jnp.bfloat16)], axis=0)
    outgoing = lax.dynamic_slice_in_dim(padded, first_column, column_count, 1)[slot_token]
    outgoing = outgoing.reshape(ep_count, local_experts, capacity, outgoing.shape[1])
    arrived = lax.all_to_all(outgoing, "ep", split_axis=0, concat_axis=0, tiled=True)
    arrived = lax.all_gather(arrived, "tp", axis=3, tiled=True)
    gate_val = jnp.einsum(
        "aecd,edf->aecf", arrived, expert_gate, preferred_element_type=jnp.float32
    )
    up_val = jnp.einsum("aecd,edf->aecf", arrived, expert_up, preferred_element_type=jnp.float32)
    hidden = (jax.nn.silu(gate_val) * up_val).astype(jnp.bfloat16)
    hidden = collect(hidden, "tp", 3)
    result = jnp.einsum(
        "aecf,efd->aecd", hidden, expert_down, preferred_element_type=jnp.float32
    ).astype(jnp.bfloat16)
    returned = lax.all_to_all(result, "ep", split_axis=0, concat_axis=0, tiled=True)
    picked = returned.reshape(expert_count * capacity, column_count)[slot_index]
    picked = picked.astype(jnp.float32).reshape(token_count, top_count, column_count)
    routed = jnp.sum(picked * route_weight[:, :, None], axis=1)
    shared_hidden = (
        jax.nn.silu(jnp.dot(normed, shared_gate, preferred_element_type=jnp.float32))
        * jnp.dot(normed, shared_up, preferred_element_type=jnp.float32)
    ).astype(jnp.bfloat16)
    shared_all = lax.all_gather(shared_hidden, "tp", axis=1, tiled=True)
    moe_total = routed + jnp.dot(shared_all, shared_down, preferred_element_type=jnp.float32)
    return (mixer_out, moe_total.astype(jnp.bfloat16))


def solution(mesh):
    placed = (
        P("ep", "tp"),
        P("ep", "tp"),
        P("ep", "tp"),
        P("tp", None),
        P(None, "tp"),
        P("ep", None),
        P(),
        P("ep", None),
        P("ep", None),
        P("ep", None, "tp"),
        P("ep", None, "tp"),
        P("ep", None, "tp"),
        P(None, "tp"),
        P(None, "tp"),
        P(None, "tp"),
    )
    return jax.shard_map(
        local, mesh=mesh, in_specs=placed, out_specs=(P("ep", "tp"), P("ep", "tp")), check_vma=False
    )
```
